32 devices in a mesh: rep: 2 (over x), fs: 8 (over z, y), tp: 2 (over core).
Axes of the slice: x: 2, y: 2, z: 4, core: 2. Of those that a mesh axis runs over, the one named last changes fastest.
Arguments:
- tokens: bfloat16 [16384, 2048], P(('rep', 'fs', 'tp')), may hold values from -6 to 6
- mix_gain: float32 [2048], replicated, may hold values from 0.1 to 1.9
- query_weight: bfloat16 [2048, 2048], P('fs', 'tp'), may hold values from -0.125 to 0.125
- key_weight: bfloat16 [2048, 2048], P('fs', 'tp'), may hold values from -0.125 to 0.125
- value_weight: bfloat16 [2048, 2048], P('fs', 'tp'), may hold values from -0.125 to 0.125
- gate_weight: bfloat16 [2048, 2048], P('fs', 'tp'), may hold values from -0.125 to 0.125
- out_weight: bfloat16 [2048, 2048], P('fs', 'tp'), may hold values from -0.125 to 0.125
- head_gain: float32 [2048], replicated, may hold values from 0.1 to 1.9
- channel_gain: float32 [2048], replicated, may hold values from 0.1 to 1.9
- inner_gate: bfloat16 [2048, 6144], P('fs', 'tp'), may hold values from -0.125 to 0.125
- inner_lift: bfloat16 [2048, 6144], P('fs', 'tp'), may hold values from -0.125 to 0.125
- inner_down: bfloat16 [2048, 6144], P('fs', 'tp'), may hold values from -0.078125 to 0.078125
- filter_taps: float32 [3, 6144], replicated, may hold values from -3.5 to 3.5
- filter_bias: float32 [6144], replicated, may hold values from -3 to 3
Outputs:
- result: bfloat16 [16384, 2048], P(('rep', 'fs', 'tp'))
The draws below stay inside these ranges and needn't reach their ends.
All inputs are finite; a program needn't handle non-finite values.
Results may differ from the reference program's by a relative error of at most 0.017.
Values may be sent and summed in bfloat16 or wider, within the bound.
A program may use at most 128 MiB of HBM per device.

```python
import jax
import jax.numpy as jnp
from jax import lax

D = 2048
HEADS = 8
HEAD_DIM = 256
FF = 6144
SEQ = 1024
BLOCK = 128
TAPS = 3
RW = 2048
TOKENS = 16384
N_TP = 2


def block_scale(rng, dims, shards, least, largest):
    def one(axis_at, shards_of):
        draws = jax.random.uniform(jax.random.fold_in(jax.random.fold_in(rng, 6), axis_at), (shards_of,), jnp.float32, least / len(shards), largest / len(shards))
        return jnp.repeat(jnp.exp(draws), dims[axis_at] // shards_of).reshape((-1,) + (1,) * (len(dims) - axis_at - 1))

    factor_of = one(*shards[0])
    for cut in shards[1:]:
        factor_of = factor_of * one(*cut)
    return factor_of


def noise(rng, shape, spread, limit, cuts=(), held_as=jnp.bfloat16):
    result = jax.random.normal(rng, shape, jnp.float32) * spread
    if len(cuts) > 0:
        result = block_scale(rng, shape, cuts, -0.22, 0.18) * result
    return jnp.clip(result, min=-limit, max=limit).astype(held_as)


def setup_inputs(seed: int = 0) -> dict:
    key_of = jax.random.split(jax.random.key(seed), 15)
    return {
        "tokens": noise(key_of[0], (TOKENS, D), 1.0, 6.0, ((0, 32),)),
        "mix_gain": jnp.clip(1.0 + 0.18 * jax.random.normal(key_of[1], (D,), jnp.float32), 0.1, 1.9),
        "query_weight": noise(key_of[2], (D, RW), D ** -0.5, 0.125, ((0, 8), (1, 2))),
        "key_weight": noise(key_of[3], (D, RW), D ** -0.5, 0.125, ((0, 8), (1, 2))),
        "value_weight": noise(key_of[4], (D, RW), D ** -0.5, 0.125, ((0, 8), (1, 2))),
        "gate_weight": noise(key_of[5], (D, RW), D ** -0.5, 0.125, ((0, 8), (1, 2))),
        "out_weight": noise(key_of[6], (D, RW), RW ** -0.5, 0.125, ((0, 8), (1, 2))),
        "head_gain": jnp.clip(1.0 + 0.18 * jax.random.normal(key_of[7], (RW,), jnp.float32), 0.1, 1.9),
        "channel_gain": jnp.clip(1.0 + 0.18 * jax.random.normal(key_of[8], (D,), jnp.float32), 0.1, 1.9),
        "inner_gate": noise(key_of[9], (D, FF), D ** -0.5, 0.125, ((0, 8), (1, 2))),
        "inner_lift": noise(key_of[10], (D, FF), D ** -0.5, 0.125, ((0, 8), (1, 2))),
        "inner_down": noise(key_of[11], (D, FF), FF ** -0.5, 0.078125, ((0, 8), (1, 2))),
        "filter_taps": noise(key_of[12], (TAPS, FF), TAPS ** -0.5, 3.5, (), jnp.float32),
        "filter_bias": noise(key_of[13], (FF,), 0.5, 3.0, (), jnp.float32),
    }


norm_eps = 1e-06
head_eps = 1.0
rope_base = 10000.0

def rms_scale(features, gain_row):
    mean_square = lax.optimization_barrier(jnp.mean(features * features, axis=-1, keepdims=True))
    return features * lax.rsqrt(mean_square + norm_eps) * gain_row

def rotate(heads_in, positions):
    half_width = heads_in.shape[-1] // 2
    inverse = rope_base ** (-jnp.arange(half_width, dtype=jnp.float32) / half_width)
    angles = positions[:, None] * inverse[None, :]
    cosine = jnp.cos(angles)[:, None, :]
    sine_part = jnp.sin(angles)[:, None, :]
    front_half = heads_in[..., :half_width]
    back_half = heads_in[..., half_width:]
    return jnp.concatenate([front_half * cosine - back_half * sine_part, front_half * sine_part + back_half * cosine], axis=-1)

def retain(queries, key_rows, value_rows, log_gamma, span):
    full_length, head_count, head_width = queries.shape
    blocks = full_length // span
    offsets = jnp.arange(span, dtype=jnp.float32)
    distance = offsets[:, None] - offsets[None, :]
    inside_segment_decay = jnp.where(distance[None] >= 0, jnp.exp(jnp.maximum(distance, 0.0)[None] * log_gamma[:, None, None]), 0.0)
    query_decay = jnp.exp((offsets[None, :] + 1.0) * log_gamma[:, None])
    key_decay_factor = jnp.exp((span - 1.0 - offsets[None, :]) * log_gamma[:, None])
    span_decay = jnp.exp(span * log_gamma)

    def to_spans(array):
        return array.reshape(blocks, span, head_count, head_width).transpose(0, 2, 1, 3)

    def advance(carry_state, inputs):
        query_segment, key_segment, value_span = inputs
        query_wide_precision = query_segment.astype(jnp.float32)
        key_wide_precision = key_segment.astype(jnp.float32)
        value_wide_precision = value_span.astype(jnp.float32)
        attention_scores = jnp.einsum('pol,pel->poe', query_wide_precision, key_wide_precision, precision=lax.Precision.HIGHEST) * inside_segment_decay
        span_weights = attention_scores.astype(jnp.bfloat16).astype(jnp.float32)
        within_span = jnp.einsum('hnm,hme->hne', span_weights, value_wide_precision, precision=lax.Precision.HIGHEST)
        carried = jnp.einsum('hnd,hde->hne', query_wide_precision, carry_state, precision=lax.Precision.HIGHEST) * query_decay[:, :, None]
        state_update = jnp.einsum('lqc,lqu->lcu', key_wide_precision * key_decay_factor[:, :, None], value_wide_precision, precision=lax.Precision.HIGHEST)
        return (carry_state * span_decay[:, None, None] + state_update, within_span + carried)
    initial = jnp.zeros((head_count, head_width, head_width), jnp.float32)
    unused, outputs = lax.scan(advance, initial, (to_spans(queries), to_spans(key_rows), to_spans(value_rows)))
    return outputs.transpose(0, 2, 1, 3).reshape(full_length, head_count, head_width)

def project(normed, weight):
    return jnp.dot(normed, weight, preferred_element_type=jnp.float32).astype(jnp.bfloat16)

def group_sum(hidden, weight, groups):
    seq_rows, columns = hidden.shape
    part_hidden = hidden.reshape(seq_rows, groups, columns // groups).astype(jnp.float32)
    part_weight = weight.reshape(weight.shape[0], groups, columns // groups).astype(jnp.float32)
    partial_value = jnp.einsum('sgc,dgc->gsd', part_hidden, part_weight, precision=lax.Precision.HIGHEST)
    rounded = lax.optimization_barrier(partial_value.astype(jnp.bfloat16))
    return lax.optimization_barrier(jnp.sum(rounded.astype(jnp.float32), axis=0))

def reference(tokens, mix_gain, query_weight, key_weight, value_weight, gate_weight, out_weight, head_gain, channel_gain, inner_gate, inner_lift, inner_down, filter_taps, filter_bias):
    head_ids = jnp.arange(HEADS, dtype=jnp.float32)
    log_gamma = jnp.log(1.0 - 2.0 ** (-5.0 - head_ids))
    positions = jnp.arange(SEQ, dtype=jnp.float32)

    def one_sequence(seq_rows):
        normed_in = rms_scale(seq_rows.astype(jnp.float32), mix_gain).astype(jnp.bfloat16)
        queries = project(normed_in, query_weight)
        key_rows = project(normed_in, key_weight)
        value_rows = project(normed_in, value_weight)
        gate_in = project(normed_in, gate_weight)
        q_rot = (rotate(queries.astype(jnp.float32).reshape(SEQ, HEADS, HEAD_DIM), positions) * HEAD_DIM ** (-0.5)).astype(jnp.bfloat16)
        k_rot = rotate(key_rows.astype(jnp.float32).reshape(SEQ, HEADS, HEAD_DIM), positions).astype(jnp.bfloat16)
        retained = retain(q_rot, k_rot, value_rows.reshape(SEQ, HEADS, HEAD_DIM), log_gamma, BLOCK)
        mean_square = lax.optimization_barrier(jnp.mean(retained * retained, axis=-1, keepdims=True))
        head_normed = (retained * lax.rsqrt(mean_square + head_eps)).reshape(SEQ, HEADS * HEAD_DIM) * head_gain
        mixed = (jax.nn.silu(gate_in.astype(jnp.float32)) * head_normed).astype(jnp.bfloat16)
        middle = seq_rows.astype(jnp.float32) + group_sum(mixed, out_weight, N_TP)
        normed_mid = rms_scale(middle, channel_gain).astype(jnp.bfloat16)
        gate_pre = project(normed_mid, inner_gate)
        lifted = project(normed_mid, inner_lift)
        padded = jnp.pad(gate_pre.astype(jnp.float32), ((TAPS - 1, 0), (0, 0)))
        filtered = filter_bias[None, :]
        for offset in range(TAPS):
            filtered = filtered + padded[offset:offset + SEQ] * filter_taps[offset][None, :]
        hidden = (jax.nn.silu(filtered) * lifted.astype(jnp.float32)).astype(jnp.bfloat16)
        return (middle + group_sum(hidden, inner_down, N_TP)).astype(jnp.bfloat16)
    sequences = tokens.reshape(TOKENS // SEQ, SEQ, D)
    return lax.map(one_sequence, sequences).reshape(TOKENS, D)
```

```python
import jax
import jax.numpy as jnp
from jax import lax
from jax.experimental import pallas as pl
from jax.experimental.pallas import tpu as pltpu
from jax.sharding import PartitionSpec as P


HEAD_DIM = 256
BLOCK = 128
TAPS = 3


norm_eps = 1e-06
head_eps = 1.0
rope_base = 10000.0


def rms_scale(features, gain_row):
    mean_square = jnp.mean(features * features, axis=-1, keepdims=True)
    return features * lax.rsqrt(mean_square + norm_eps) * gain_row


def rotate(heads_in, positions):
    half_width = heads_in.shape[-1] // 2
    inverse = rope_base ** (-jnp.arange(half_width, dtype=jnp.float32) / half_width)
    angles = positions[:, None] * inverse[None, :]
    cosine = jnp.cos(angles)[:, None, :]
    sine_part = jnp.sin(angles)[:, None, :]
    front_half = heads_in[..., :half_width]
    back_half = heads_in[..., half_width:]
    return jnp.concatenate(
        [front_half * cosine - back_half * sine_part, front_half * sine_part + back_half * cosine],
        axis=-1,
    )


def retain(queries, key_rows, value_rows, log_gamma, span):
    full_length, head_count, head_width = queries.shape
    blocks = full_length // span
    offsets = jnp.arange(span, dtype=jnp.float32)
    distance = offsets[:, None] - offsets[None, :]
    inside_segment_decay = jnp.where(
        distance[None] >= 0,
        jnp.exp(jnp.maximum(distance, 0.0)[None] * log_gamma[:, None, None]),
        0.0,
    )
    query_decay = jnp.exp((offsets[None, :] + 1.0) * log_gamma[:, None])
    key_decay_factor = jnp.exp((span - 1.0 - offsets[None, :]) * log_gamma[:, None])
    span_decay = jnp.exp(span * log_gamma)

    def to_spans(array):
        return array.reshape(blocks, span, head_count, head_width).transpose(0, 2, 1, 3)

    def advance(carry_state, inputs):
        query_segment, key_segment, value_span = inputs
        attention_scores = (
            jnp.einsum(
                "pol,pel->poe", query_segment, key_segment, preferred_element_type=jnp.float32
            )
            * inside_segment_decay
        )
        span_weights = attention_scores.astype(jnp.bfloat16)
        within_span = jnp.einsum(
            "hnm,hme->hne", span_weights, value_span, preferred_element_type=jnp.float32
        )
        carried = (
            jnp.einsum(
                "hnd,hde->hne",
                query_segment.astype(jnp.float32),
                carry_state,
                precision=lax.Precision.HIGHEST,
            )
            * query_decay[:, :, None]
        )
        state_update = jnp.einsum(
            "lqc,lqu->lcu",
            key_segment.astype(jnp.float32) * key_decay_factor[:, :, None],
            value_span.astype(jnp.float32),
            precision=lax.Precision.HIGHEST,
        )
        return (carry_state * span_decay[:, None, None] + state_update, within_span + carried)

    initial = jnp.zeros((head_count, head_width, head_width), jnp.float32)
    _, outputs = lax.scan(
        advance, initial, (to_spans(queries), to_spans(key_rows), to_spans(value_rows))
    )
    return outputs.transpose(0, 2, 1, 3).reshape(full_length, head_count, head_width)


def transposed_product(rows_in, weight):
    return lax.dot_general(
        rows_in, weight, (((1,), (1,)), ((), ())), preferred_element_type=jnp.float32
    )


def shift_pairs(groups, step):
    return [(source, (source + step) % groups) for source in range(groups)]


def gather_rows(rows, groups, index):
    rows_dev = rows.shape[0]
    whole = jnp.zeros((rows_dev * groups,) + rows.shape[1:], rows.dtype)
    whole = lax.dynamic_update_slice_in_dim(whole, rows, index * rows_dev, 0)
    for step in range(1, groups):
        arrived = lax.ppermute(rows, "tp", shift_pairs(groups, step))
        owner = (index - step + groups) % groups
        whole = lax.dynamic_update_slice_in_dim(whole, arrived, owner * rows_dev, 0)
    return whole


def sum_groups(partial, groups):
    total = partial.astype(jnp.float32)
    for step in range(1, groups):
        arrived = lax.ppermute(partial, "tp", shift_pairs(groups, step))
        total = total + arrived.astype(jnp.float32)
    return total


def scatter_groups(partial, groups, index):
    rows_dev = partial.shape[0] // groups
    total = lax.dynamic_slice_in_dim(partial, index * rows_dev, rows_dev, 0).astype(jnp.float32)
    for step in range(1, groups):
        target = (index + step) % groups
        leaving = lax.dynamic_slice_in_dim(partial, target * rows_dev, rows_dev, 0)
        arrived = lax.ppermute(leaving, "tp", shift_pairs(groups, step))
        total = total + arrived.astype(jnp.float32)
    return total


def shared_width(columns, unit, numerator, denominator):
    if lax.axis_size("rep") != 2:
        return 0
    return (columns // unit) * numerator // denominator * unit


def column_pieces(array, width):
    columns = array.shape[-1]
    if width == 0:
        return [array]
    rep_index = lax.axis_index("rep")
    pieces = [lax.dynamic_slice_in_dim(array, rep_index * (columns - width), width, array.ndim - 1)]
    if columns > 2 * width:
        pieces.append(array[..., width : columns - width])
    pieces.append(
        lax.dynamic_slice_in_dim(
            array, (1 - rep_index) * (columns - width), width, array.ndim - 1
        )
    )
    return pieces


def gather_weights(weights, width):
    columns = weights[0].shape[1]
    if width == 0:
        return [[lax.all_gather(weight, "fs", axis=0, tiled=True)] for weight in weights]
    rep_index = lax.axis_index("rep")
    start = rep_index * (columns - width)
    count = len(weights)

    def cut(whole):
        each = whole.shape[1] // count
        return [whole[:, order * each : (order + 1) * each] for order in range(count)]

    own = join([lax.dynamic_slice_in_dim(weight, start, width, 1) for weight in weights])
    first = lax.all_gather(own, "fs", axis=0, tiled=True)
    pieces = [cut(first)]
    if columns > 2 * width:
        common = join([weight[:, width : columns - width] for weight in weights])
        pieces.append(cut(lax.all_gather(common, "fs", axis=0, tiled=True)))
    pieces.append(cut(lax.ppermute(first, "rep", [(0, 1), (1, 0)])))
    return [list(each) for each in zip(*pieces)]


def product(rows_in, weight):
    return jnp.dot(rows_in, weight, preferred_element_type=jnp.float32).astype(jnp.bfloat16)


def join(pieces):
    return pieces[0] if len(pieces) == 1 else jnp.concatenate(pieces, axis=-1)


def shards_any(
    tokens,
    mix_gain,
    query_weight,
    key_weight,
    value_weight,
    gate_weight,
    out_weight,
    head_gain,
    channel_gain,
    inner_gate,
    inner_lift,
    inner_down,
    filter_taps,
    filter_bias,
):
    tp_index = lax.axis_index("tp")
    groups = lax.axis_size("tp")
    rows_dev = tokens.shape[0]
    cols_dev = query_weight.shape[1]
    hidden_dev = inner_gate.shape[1]
    heads_dev = cols_dev // HEAD_DIM
    full_length = rows_dev * groups
    head_width = shared_width(cols_dev, HEAD_DIM, 1, 2)
    hidden_width = shared_width(hidden_dev, 128, 1, 3)
    query_set, key_set = gather_weights([query_weight, key_weight], head_width)
    value_set, gate_set = gather_weights([value_weight, gate_weight], head_width)
    (out_set,) = gather_weights([out_weight], head_width)
    inner_gate_set, inner_lift_set = gather_weights([inner_gate, inner_lift], hidden_width)
    (down_set,) = gather_weights([inner_down], hidden_width)
    whole_tokens = gather_rows(tokens, groups, tp_index)
    normed_whole = lax.optimization_barrier(
        rms_scale(whole_tokens.astype(jnp.float32), mix_gain).astype(jnp.bfloat16)
    )
    queries = join([product(normed_whole, piece) for piece in query_set])
    key_rows = join([product(normed_whole, piece) for piece in key_set])
    value_rows = join([product(normed_whole, piece) for piece in value_set])
    gate_in = join([product(normed_whole, piece) for piece in gate_set])
    positions = jnp.arange(full_length, dtype=jnp.float32)
    q_rot = (
        rotate(queries.astype(jnp.float32).reshape(full_length, heads_dev, HEAD_DIM), positions)
        * HEAD_DIM ** (-0.5)
    ).astype(jnp.bfloat16)
    k_rot = rotate(
        key_rows.astype(jnp.float32).reshape(full_length, heads_dev, HEAD_DIM), positions
    ).astype(jnp.bfloat16)
    head_order = join(
        column_pieces(jnp.arange(heads_dev, dtype=jnp.int32), head_width // HEAD_DIM)
    )
    head_ids = (tp_index * heads_dev + head_order).astype(jnp.float32)
    log_gamma = jnp.log(1.0 - 2.0 ** (-5.0 - head_ids))
    retained = retain(
        q_rot, k_rot, value_rows.reshape(full_length, heads_dev, HEAD_DIM), log_gamma, BLOCK
    )
    mean_square = jnp.mean(retained * retained, axis=-1, keepdims=True)
    gain_dev = lax.dynamic_slice_in_dim(head_gain, tp_index * cols_dev, cols_dev, 0)
    gain_dev = join(column_pieces(gain_dev, head_width))
    head_normed = (retained * lax.rsqrt(mean_square + head_eps)).reshape(
        full_length, cols_dev
    ) * gain_dev
    mixed = (jax.nn.silu(gate_in.astype(jnp.float32)) * head_normed).astype(jnp.bfloat16)
    out_product = 0.0
    column = 0
    for piece in out_set:
        part = mixed[:, column : column + piece.shape[1]]
        out_product = out_product + transposed_product(part, piece)
        column += piece.shape[1]
    mixer_whole = sum_groups(out_product.astype(jnp.bfloat16), groups)
    middle_whole = whole_tokens.astype(jnp.float32) + mixer_whole
    normed_mid = lax.optimization_barrier(
        rms_scale(middle_whole, channel_gain).astype(jnp.bfloat16)
    )
    middle = lax.dynamic_slice_in_dim(middle_whole, tp_index * rows_dev, rows_dev, 0)
    taps_dev = lax.dynamic_slice_in_dim(filter_taps, tp_index * hidden_dev, hidden_dev, 1)
    bias_dev = lax.dynamic_slice_in_dim(filter_bias, tp_index * hidden_dev, hidden_dev, 0)
    taps_set = column_pieces(taps_dev, hidden_width)
    bias_set = column_pieces(bias_dev, hidden_width)
    down_product = 0.0
    for gate_piece, lift_piece, down_piece, taps_piece, bias_piece in zip(
        inner_gate_set, inner_lift_set, down_set, taps_set, bias_set
    ):
        gate_pre = product(normed_mid, gate_piece)
        lifted = product(normed_mid, lift_piece)
        padded = jnp.pad(gate_pre, ((TAPS - 1, 0), (0, 0)))
        filtered = bias_piece[None, :]
        for offset in range(TAPS):
            shifted = padded[offset : offset + full_length].astype(jnp.float32)
            filtered = filtered + shifted * taps_piece[offset][None, :]
        hidden = (jax.nn.silu(filtered) * lifted.astype(jnp.float32)).astype(jnp.bfloat16)
        down_product = down_product + transposed_product(hidden, down_piece)
    outcome = middle + scatter_groups(down_product.astype(jnp.bfloat16), groups, tp_index)
    return outcome.astype(jnp.bfloat16)


def ring_pairs(count):
    order = list(range(0, count, 2)) + list(range(count - 1, 0, -2))
    return order, [(order[at], order[(at + 1) % count]) for at in range(count)]


def after(array, *earlier):
    return lax.optimization_barrier((array,) + earlier)[0]


class Ring:
    def __init__(self, shard, count, far_way):
        _, ahead = ring_pairs(count)
        behind = [(target, source) for source, target in ahead]
        self.blocks = {0: shard}
        self.hops = []
        up = down = shard
        for step in range(1, count // 2 + 1):
            arrived = []
            for way in ways(step, count, far_way):
                if way == "up":
                    up = lax.ppermute(up, "fs", ahead)
                    self.blocks[count - step] = up
                    arrived.append(up)
                else:
                    down = lax.ppermute(down, "fs", behind)
                    self.blocks[step] = down
                    arrived.append(down)
            self.hops.append(tuple(arrived))

    def parts(self, distances):
        return [self.blocks[at] for at in distances]


def ways(step, count, far_way):
    return ("up", "down") if step < count // 2 else (far_way,)


FAR_WAY = {"ra": "up", "rb": "down", "rg": "up", "rl": "down", "rc": "up", "rd": "down"}


def swap(array, axis):
    return lax.ppermute(array, axis, [(0, 1), (1, 0)])


def retain_kernel(
    swapped_ref,
    log_gamma_ref,
    query_ref,
    key_ref,
    value_ref,
    gate_ref,
    cosine_ref,
    sine_ref,
    gain_ref,
    mixed_ref,
):
    log_gamma = log_gamma_ref[pl.program_id(0)]
    length, width = query_ref.shape
    late = swapped_ref[0] * (length // 2)
    half = width // 2
    span = BLOCK
    rows = lax.broadcasted_iota(jnp.int32, (span, span), 0)
    columns = lax.broadcasted_iota(jnp.int32, (span, span), 1)
    distance = (rows - columns).astype(jnp.float32)
    inside = jnp.where(distance >= 0, jnp.exp(jnp.maximum(distance, 0.0) * log_gamma), 0.0)
    offsets = lax.broadcasted_iota(jnp.int32, (span, width), 0).astype(jnp.float32)
    query_decay = jnp.exp((offsets + 1.0) * log_gamma)
    key_decay = jnp.exp((span - 1.0 - offsets) * log_gamma)
    span_decay = jnp.exp(jnp.full((width, width), span, jnp.float32) * log_gamma)
    gain = gain_ref[...]

    def turn(ref, at, stored, scale):
        rows_in = ref[stored, :].astype(jnp.float32)
        front, back = rows_in[:, :half], rows_in[:, half:]
        cosine = cosine_ref[pl.ds(at, span), :]
        sine = sine_ref[pl.ds(at, span), :]
        turned = jnp.concatenate(
            [front * cosine - back * sine, front * sine + back * cosine], axis=-1
        )
        return (turned * scale).astype(jnp.bfloat16)

    def both(wide):
        high = wide.astype(jnp.bfloat16)
        return high, (wide - high.astype(jnp.float32)).astype(jnp.bfloat16)

    def dot(left, right, left_axis, right_axis):
        return lax.dot_general(
            left,
            right,
            (((left_axis,), (right_axis,)), ((), ())),
            preferred_element_type=jnp.float32,
        )

    state = jnp.zeros((width, width), jnp.float32)
    for block in range(length // span):
        at = block * span
        first = at + late if at < length // 2 else at - late
        stored = pl.ds(pl.multiple_of(first, span), span)
        query = turn(query_ref, at, stored, HEAD_DIM ** (-0.5))
        key = turn(key_ref, at, stored, 1.0)
        value = value_ref[stored, :]
        weights = (dot(query, key, 1, 1) * inside).astype(jnp.bfloat16)
        retained = dot(weights, value, 1, 0)
        if block > 0:
            high, low = both(state)
            retained = retained + (dot(query, high, 1, 0) + dot(query, low, 1, 0)) * query_decay
        if block < length // span - 1:
            high, low = both(key.astype(jnp.float32) * key_decay)
            added = dot(high, value, 0, 0) + dot(low, value, 0, 0)
            state = state * span_decay + added
        mean_square = jnp.mean(retained * retained, axis=-1, keepdims=True)
        normed = retained * lax.rsqrt(mean_square + head_eps) * gain
        gate = gate_ref[stored, :].astype(jnp.float32)
        mixed_ref[stored, :] = (gate * jax.nn.sigmoid(gate) * normed).astype(jnp.bfloat16)


def mix_heads(query_key, value_gate, cosine, sine, gain, log_gamma, swapped):
    length, columns = value_gate.shape[0], query_key.shape[1] // 2
    heads = columns // HEAD_DIM
    front = pl.BlockSpec((length, HEAD_DIM), lambda head, *_: (0, head))
    back = pl.BlockSpec((length, HEAD_DIM), lambda head, *_: (0, head + heads))
    table = pl.BlockSpec((length, HEAD_DIM // 2), lambda head, *_: (0, 0))
    return pl.pallas_call(
        retain_kernel,
        out_shape=jax.ShapeDtypeStruct((length, columns), jnp.bfloat16),
        grid_spec=pltpu.PrefetchScalarGridSpec(
            num_scalar_prefetch=2,
            grid=(heads,),
            in_specs=[front, back, front, back, table, table]
            + [pl.BlockSpec((1, HEAD_DIM), lambda head, *_: (0, head))],
            out_specs=front,
        ),
        compiler_params=pltpu.CompilerParams(vmem_limit_bytes=VMEM_LIMIT),
        cost_estimate=pl.CostEstimate(
            flops=length * columns * (4 * BLOCK + 8 * HEAD_DIM) * 4,
            bytes_accessed=length * columns * 10,
            transcendentals=length * columns,
        ),
    )(swapped, log_gamma, query_key, query_key, value_gate, value_gate, cosine, sine, gain.reshape(1, -1))


VMEM_LIMIT = 26 * 2**20


def stacked(refs):
    return jnp.concatenate([ref[...] for ref in refs], axis=0)


def whole_block(array):
    return pl.BlockSpec(
        array.shape, lambda at: (0,) * array.ndim, pipeline_mode=pl.Buffered(1)
    )


def strip(array, width):
    return pl.BlockSpec((array.shape[0], width), lambda at: (0, at))


def project_rows(row_parts, weight_blocks, columns, width=256):
    count = len(row_parts)
    part_rows, depth = row_parts[0].shape
    width = min(width, columns)

    def body(*refs):
        weight = stacked(refs[count:-1])
        for at in range(count):
            refs[-1][pl.ds(at * part_rows, part_rows), :] = jnp.dot(
                refs[at][...], weight, preferred_element_type=jnp.float32
            ).astype(jnp.bfloat16)

    return pl.pallas_call(
        body,
        out_shape=jax.ShapeDtypeStruct((count * part_rows, columns), jnp.bfloat16),
        grid=(columns // width,),
        in_specs=[whole_block(part) for part in row_parts]
        + [strip(block, width) for block in weight_blocks],
        out_specs=pl.BlockSpec((count * part_rows, width), lambda at: (0, at)),
        compiler_params=pltpu.CompilerParams(vmem_limit_bytes=VMEM_LIMIT),
        cost_estimate=pl.CostEstimate(
            flops=2 * count * part_rows * depth * columns,
            bytes_accessed=2 * (count * part_rows * (depth + columns) + depth * columns),
            transcendentals=0,
        ),
    )(*row_parts, *weight_blocks)


def project_back(depth_parts, weight_blocks, first_strip=0, tile=256):
    count = len(depth_parts)
    rows, strip_depth = depth_parts[0].shape
    columns = sum(block.shape[0] for block in weight_blocks)
    part_rows = rows // 2
    tiles = part_rows // tile
    first = first_strip // count

    def body(*refs):
        rows_in = jnp.concatenate([ref[...] for ref in refs[:count]], axis=1)
        product_tile = transposed_product(rows_in, stacked(refs[count:-2])).astype(jnp.bfloat16)

        @pl.when(pl.program_id(0) < tiles)
        def _():
            refs[-2][...] = product_tile

        @pl.when(pl.program_id(0) >= tiles)
        def _():
            refs[-1][...] = product_tile

    part = jax.ShapeDtypeStruct((part_rows, columns), jnp.bfloat16)
    return pl.pallas_call(
        body,
        out_shape=(part, part),
        grid=(2 * tiles,),
        in_specs=[pl.BlockSpec((tile, strip_depth), lambda at: (at, 0))] * count
        + [
            pl.BlockSpec(
                (block.shape[0], count * strip_depth),
                lambda at: (0, first),
                pipeline_mode=pl.Buffered(1),
            )
            for block in weight_blocks
        ],
        out_specs=(
            pl.BlockSpec((tile, columns), lambda at: (jnp.minimum(at, tiles - 1), 0)),
            pl.BlockSpec((tile, columns), lambda at: (jnp.maximum(at - tiles, 0), 0)),
        ),
        compiler_params=pltpu.CompilerParams(vmem_limit_bytes=VMEM_LIMIT),
        cost_estimate=pl.CostEstimate(
            flops=2 * rows * count * strip_depth * columns,
            bytes_accessed=2 * (rows * columns + count * strip_depth * (rows + columns)),
            transcendentals=0,
        ),
    )(*depth_parts, *weight_blocks)


def hidden_rows(mine, theirs, gate_blocks, lift_blocks, taps, bias, swapped, share, shares):
    part_rows, depth = mine.shape
    columns = gate_blocks[0].shape[1] // shares
    count = len(gate_blocks)
    width = next(width for width in (512, 384, 256, 128) if columns % width == 0)
    first_strip = share * (columns // width)

    chunk = 128

    def body(swapped_ref, mine_ref, theirs_ref, *refs):
        taps_ref, bias_ref, hidden_ref = refs[2 * count :]
        gate_weight, lift_weight = stacked(refs[:count]), stacked(refs[count : 2 * count])

        def rounded(rows_in, weight):
            wide = jnp.dot(rows_in, weight, preferred_element_type=jnp.float32)
            return wide.astype(jnp.bfloat16).astype(jnp.float32)

        def hidden_of(before, pre, lifted):
            padded = jnp.concatenate([before, pre], axis=0)
            filtered = bias_ref[...]
            for offset in range(TAPS):
                start = 8 - (TAPS - 1) + offset
                filtered = filtered + padded[start : start + pre.shape[0]] * taps_ref[offset : offset + 1, :]
            return (filtered * jax.nn.sigmoid(filtered) * lifted).astype(jnp.bfloat16)

        before = jnp.zeros((8, width), jnp.float32)
        for at, ref in enumerate((mine_ref, theirs_ref)):
            if at == 1:
                before = jnp.where(swapped_ref[0] == 0, before, 0.0)
            for first in range(0, part_rows, chunk):
                rows_in = ref[pl.ds(first, chunk), :]
                pre = rounded(rows_in, gate_weight)
                lifted = rounded(rows_in, lift_weight)
                hidden_ref[pl.ds(at * part_rows + first, chunk), :] = hidden_of(before, pre, lifted)
                before = pre[chunk - 8 :]
                if at == 0 and first == 0:
                    opening = pre[:16], lifted[:16]
        before = jnp.where(swapped_ref[0] == 1, before, 0.0)
        hidden_ref[pl.ds(0, 16), :] = hidden_of(before, *opening)

    def strip_at(rows, ahead=first_strip):
        return pl.BlockSpec((rows, width), lambda at, *_: (0, at + ahead))

    rows_spec = pl.BlockSpec(
        (part_rows, depth), lambda at, *_: (0, 0), pipeline_mode=pl.Buffered(1)
    )
    return pl.pallas_call(
        body,
        out_shape=jax.ShapeDtypeStruct((2 * part_rows, columns), jnp.bfloat16),
        grid_spec=pltpu.PrefetchScalarGridSpec(
            num_scalar_prefetch=1,
            grid=(columns // width,),
            in_specs=[rows_spec, rows_spec]
            + [strip_at(block.shape[0]) for block in gate_blocks + lift_blocks]
            + [strip_at(TAPS), strip_at(1)],
            out_specs=strip_at(2 * part_rows, 0),
        ),
        compiler_params=pltpu.CompilerParams(vmem_limit_bytes=VMEM_LIMIT),
        cost_estimate=pl.CostEstimate(
            flops=8 * part_rows * depth * columns,
            bytes_accessed=4 * (part_rows * (depth + columns) + depth * columns),
            transcendentals=2 * part_rows * columns,
        ),
    )(swapped, mine, theirs, *gate_blocks, *lift_blocks, taps, bias)


def by_row_tiles(body, owners, arrays, wide, outputs, tile=128):
    rows = arrays[0].shape[0]

    def tiled(array):
        return pl.BlockSpec((tile, array.shape[1]), lambda at, *_: (at, 0))

    return pl.pallas_call(
        body,
        out_shape=outputs,
        grid_spec=pltpu.PrefetchScalarGridSpec(
            num_scalar_prefetch=1,
            grid=(rows // tile,),
            in_specs=[tiled(array) for array in arrays]
            + [pl.BlockSpec(array.shape, lambda at, *_: (0, 0)) for array in wide],
            out_specs=[tiled(array) for array in outputs],
        ),
        compiler_params=pltpu.CompilerParams(vmem_limit_bytes=VMEM_LIMIT),
        cost_estimate=pl.CostEstimate(
            flops=200 * rows * arrays[0].shape[1],
            bytes_accessed=4 * rows * arrays[0].shape[1] * (len(arrays) + len(outputs)) // 2,
            transcendentals=rows,
        ),
    )(owners, *arrays, *wide)


def block_of(owners_ref, distance, width):
    return pl.ds(pl.multiple_of(owners_ref[distance] * width, width), width)


def norm_input(tokens, gain, owners, count):
    rows, features = tokens.shape
    width = features // count

    def body(owners_ref, tokens_ref, gain_ref, normed_ref):
        wide = tokens_ref[...].astype(jnp.float32)
        factor = lax.rsqrt(jnp.mean(wide * wide, axis=-1, keepdims=True) + norm_eps)
        for at in range(count):
            taken = block_of(owners_ref, at, width)
            normed_ref[:, at * width : (at + 1) * width] = (
                tokens_ref[:, taken].astype(jnp.float32) * factor * gain_ref[:, taken]
            ).astype(jnp.bfloat16)

    outputs = [jax.ShapeDtypeStruct((rows, features), jnp.bfloat16)]
    return by_row_tiles(body, owners, [tokens], [gain[None, :]], outputs)[0]


def norm_middle(tokens, parts, gain, owners, count):
    rows, features = tokens.shape
    width = features // count

    def body(owners_ref, tokens_ref, mine_ref, theirs_ref, far_ref, gain_ref, middle_ref, normed_ref):
        squares = jnp.zeros((tokens_ref.shape[0], 1), jnp.float32)
        for at in range(count):
            placed = slice(at * width, (at + 1) * width)
            taken = block_of(owners_ref, at, width)
            mixer = mine_ref[:, placed].astype(jnp.float32) + theirs_ref[:, placed].astype(jnp.float32)
            mixer = mixer + far_ref[:, placed].astype(jnp.float32)
            middle = tokens_ref[:, taken].astype(jnp.float32) + mixer
            middle_ref[:, placed] = middle
            squares = squares + jnp.sum(middle * middle, axis=-1, keepdims=True)
        factor = lax.rsqrt(squares / features + norm_eps)
        for at in range(count):
            placed = slice(at * width, (at + 1) * width)
            taken = block_of(owners_ref, at, width)
            normed_ref[:, placed] = (middle_ref[:, placed] * factor * gain_ref[:, taken]).astype(
                jnp.bfloat16
            )

    outputs = [
        jax.ShapeDtypeStruct((rows, features), jnp.float32),
        jax.ShapeDtypeStruct((rows, features), jnp.bfloat16),
    ]
    return by_row_tiles(body, owners, [tokens] + parts, [gain[None, :]], outputs)


def outcome_rows(middle, group_parts, groups, owners, count):
    rows, features = middle.shape
    width = features // count
    parts = [part for group in group_parts for part in group]

    def body(owners_ref, middle_ref, *refs):
        for number, group in enumerate(groups):
            mine_ref, theirs_ref, far_ref = refs[3 * number : 3 * number + 3]
            for order, at in enumerate(group):
                placed = slice(order * width, (order + 1) * width)
                channel = mine_ref[:, placed].astype(jnp.float32) + theirs_ref[:, placed].astype(jnp.float32)
                channel = channel + far_ref[:, placed].astype(jnp.float32)
                refs[-1][:, block_of(owners_ref, at, width)] = (
                    middle_ref[:, at * width : (at + 1) * width] + channel
                ).astype(jnp.bfloat16)

    outputs = [jax.ShapeDtypeStruct((rows, features), jnp.bfloat16)]
    return by_row_tiles(body, owners, [middle] + parts, [], outputs)[0]


def shards(
    tokens,
    mix_gain,
    query_weight,
    key_weight,
    value_weight,
    gate_weight,
    out_weight,
    head_gain,
    channel_gain,
    inner_gate,
    inner_lift,
    inner_down,
    filter_taps,
    filter_bias,
):
    tp_index = lax.axis_index("tp")
    rep_index = lax.axis_index("rep")
    fs_index = lax.axis_index("fs")
    count = lax.axis_size("fs")
    odd = fs_index % 2
    place = jnp.where(odd == 0, fs_index // 2, count - 1 - fs_index // 2)
    rows_dev, _ = tokens.shape
    length = rows_dev * 2
    cols = query_weight.shape[1] // 2
    hidden_cols = inner_gate.shape[1] // 2
    heads = cols // HEAD_DIM
    every = list(range(count))
    around = (place + jnp.arange(count, dtype=jnp.int32)) % count
    owners = jnp.where(around < count // 2, 2 * around, 2 * (count - around) - 1).astype(jnp.int32)
    swapped = tp_index.reshape(1).astype(jnp.int32)

    def part(weight, columns):
        return lax.dynamic_slice_in_dim(weight, rep_index * columns, columns, weight.ndim - 1)

    def joint(pieces):
        return jnp.concatenate(pieces, axis=-1)

    ring_a = Ring(joint([part(query_weight, cols), part(key_weight, cols)]), count, FAR_WAY["ra"])
    ring_b = Ring(
        joint([part(value_weight, cols), part(gate_weight, cols), part(out_weight, cols)]),
        count,
        FAR_WAY["rb"],
    )

    ring_g = Ring(after(part(inner_gate, hidden_cols), *ring_a.hops[-1]), count, FAR_WAY["rg"])
    ring_l = Ring(after(part(inner_lift, hidden_cols), *ring_b.hops[-1]), count, FAR_WAY["rl"])
    down = part(inner_down, hidden_cols)
    down_half = down.shape[0] // 2
    ring_c = Ring(after(down[:down_half], *ring_g.hops[-1]), count, FAR_WAY["rc"])
    ring_d = Ring(after(down[down_half:], *ring_l.hops[-1]), count, FAR_WAY["rd"])

    normed = norm_input(tokens, mix_gain, owners, count)
    far = swap(normed, "rep")
    own_in = [normed, swap(normed, "tp")]
    other_in = [far, swap(far, "tp")]

    positions = jnp.arange(length, dtype=jnp.float32)
    inverse = rope_base ** (
        -jnp.arange(HEAD_DIM // 2, dtype=jnp.float32) / (HEAD_DIM // 2)
    )
    angles = positions[:, None] * inverse[None, :]
    first_head = (tp_index * 2 + rep_index) * heads
    head_ids = (first_head + jnp.arange(heads, dtype=jnp.int32)).astype(jnp.float32)
    log_gamma = jnp.log(1.0 - 2.0 ** (-5.0 - head_ids))
    gain_dev = lax.dynamic_slice_in_dim(head_gain, first_head * HEAD_DIM, cols, 0)
    tables = (jnp.cos(angles), jnp.sin(angles), gain_dev, log_gamma, swapped)
    early_blocks, late_blocks = ring_a.parts(every), ring_b.parts(every)

    def mixer_part(rows_in):
        query_key = project_rows(rows_in, early_blocks, 2 * cols)
        value_gate = project_rows(rows_in, late_blocks, 2 * cols)
        mixed = mix_heads(query_key, value_gate, *tables)
        return project_back([mixed], late_blocks, 2)

    other_mine, other_theirs = mixer_part(other_in)
    other_sum = other_mine.astype(jnp.float32) + swap(other_theirs, "tp").astype(jnp.float32)
    far = swap(other_sum.astype(jnp.bfloat16), "rep")
    own_mine, own_theirs = mixer_part(own_in)
    middle, normed_mid = norm_middle(
        tokens, [own_mine, swap(own_theirs, "tp"), far], channel_gain, owners, count
    )
    far = swap(normed_mid, "rep")
    own_mid = [normed_mid, swap(normed_mid, "tp")]
    other_mid = [far, swap(far, "tp")]

    first_hidden = (tp_index * 2 + rep_index) * hidden_cols

    taps = lax.dynamic_slice_in_dim(filter_taps, first_hidden, hidden_cols, 1)
    bias = lax.dynamic_slice_in_dim(filter_bias, first_hidden, hidden_cols, 0)[None, :]
    hidden_blocks = ring_g.parts(every), ring_l.parts(every)

    def hidden_strips(rows_in, shares):
        return [
            hidden_rows(*rows_in, *hidden_blocks, taps, bias, swapped, share, shares)
            for share in range(shares)
        ]

    own_hidden = hidden_strips(own_mid, 2)
    other_hidden = hidden_strips(other_mid, 1)
    near = count // 2 - 2
    groups = [
        [at for at in every if min(at, count - at) <= near],
        [at for at in every if min(at, count - at) > near],
    ]
    group_parts = []
    for group in groups:
        blocks = [
            piece for at in group for ring in (ring_c, ring_d) for piece in ring.parts([at])
        ]
        other_mine, other_theirs = project_back(other_hidden, blocks)
        theirs = swap(other_theirs, "tp")
        other_sum = other_mine.astype(jnp.float32) + theirs.astype(jnp.float32)
        far = swap(other_sum.astype(jnp.bfloat16), "rep")
        own_mine, own_theirs = project_back(own_hidden, blocks)
        group_parts.append([own_mine, swap(own_theirs, "tp"), far])
    return outcome_rows(middle, group_parts, groups, owners, count)


def split_pays(mesh):
    sizes = mesh.shape
    return sizes["rep"] == 2 and sizes["tp"] == 2 and sizes["fs"] % 2 == 0 and sizes["fs"] >= 8


def solution(mesh):
    in_specs = (
        P(("rep", "fs", "tp"), None),
        P(),
        P("fs", "tp"),
        P("fs", "tp"),
        P("fs", "tp"),
        P("fs", "tp"),
        P("fs", "tp"),
        P(),
        P(),
        P("fs", "tp"),
        P("fs", "tp"),
        P("fs", "tp"),
        P(),
        P(),
    )
    out_specs = P(("rep", "fs", "tp"), None)
    if not split_pays(mesh):
        return jax.shard_map(
            shards_any, mesh=mesh, in_specs=in_specs, out_specs=out_specs, check_vma=False
        )
    return jax.shard_map(shards, mesh=mesh, in_specs=in_specs, out_specs=out_specs, check_vma=False)
```

```python
import jax
import jax.numpy as jnp
from jax import lax
from jax.experimental import pallas as pl
from jax.experimental.pallas import tpu as pltpu
from jax.sharding import PartitionSpec as P


HEAD_DIM = 256
BLOCK = 128
TAPS = 3


norm_eps = 1e-06
head_eps = 1.0
rope_base = 10000.0


def rms_scale(features, gain_row):
    mean_square = jnp.mean(features * features, axis=-1, keepdims=True)
    return features * lax.rsqrt(mean_square + norm_eps) * gain_row


def rotate(heads_in, positions):
    half_width = heads_in.shape[-1] // 2
    inverse = rope_base ** (-jnp.arange(half_width, dtype=jnp.float32) / half_width)
    angles = positions[:, None] * inverse[None, :]
    cosine = jnp.cos(angles)[:, None, :]
    sine_part = jnp.sin(angles)[:, None, :]
    front_half = heads_in[..., :half_width]
    back_half = heads_in[..., half_width:]
    return jnp.concatenate(
        [front_half * cosine - back_half * sine_part, front_half * sine_part + back_half * cosine],
        axis=-1,
    )


def retain(queries, key_rows, value_rows, log_gamma, span):
    full_length, head_count, head_width = queries.shape
    blocks = full_length // span
    offsets = jnp.arange(span, dtype=jnp.float32)
    distance = offsets[:, None] - offsets[None, :]
    inside_segment_decay = jnp.where(
        distance[None] >= 0,
        jnp.exp(jnp.maximum(distance, 0.0)[None] * log_gamma[:, None, None]),
        0.0,
    )
    query_decay = jnp.exp((offsets[None, :] + 1.0) * log_gamma[:, None])
    key_decay_factor = jnp.exp((span - 1.0 - offsets[None, :]) * log_gamma[:, None])
    span_decay = jnp.exp(span * log_gamma)

    def to_spans(array):
        return array.reshape(blocks, span, head_count, head_width).transpose(0, 2, 1, 3)

    def advance(carry_state, inputs):
        query_segment, key_segment, value_span = inputs
        attention_scores = (
            jnp.einsum(
                "pol,pel->poe", query_segment, key_segment, preferred_element_type=jnp.float32
            )
            * inside_segment_decay
        )
        span_weights = attention_scores.astype(jnp.bfloat16)
        within_span = jnp.einsum(
            "hnm,hme->hne", span_weights, value_span, preferred_element_type=jnp.float32
        )
        carried = (
            jnp.einsum(
                "hnd,hde->hne",
                query_segment.astype(jnp.float32),
                carry_state,
                precision=lax.Precision.HIGHEST,
            )
            * query_decay[:, :, None]
        )
        state_update = jnp.einsum(
            "lqc,lqu->lcu",
            key_segment.astype(jnp.float32) * key_decay_factor[:, :, None],
            value_span.astype(jnp.float32),
            precision=lax.Precision.HIGHEST,
        )
        return (carry_state * span_decay[:, None, None] + state_update, within_span + carried)

    initial = jnp.zeros((head_count, head_width, head_width), jnp.float32)
    _, outputs = lax.scan(
        advance, initial, (to_spans(queries), to_spans(key_rows), to_spans(value_rows))
    )
    return outputs.transpose(0, 2, 1, 3).reshape(full_length, head_count, head_width)


def transposed_product(rows_in, weight):
    return lax.dot_general(
        rows_in, weight, (((1,), (1,)), ((), ())), preferred_element_type=jnp.float32
    )


def shift_pairs(groups, step):
    return [(source, (source + step) % groups) for source in range(groups)]


def gather_rows(rows, groups, index):
    rows_dev = rows.shape[0]
    whole = jnp.zeros((rows_dev * groups,) + rows.shape[1:], rows.dtype)
    whole = lax.dynamic_update_slice_in_dim(whole, rows, index * rows_dev, 0)
    for step in range(1, groups):
        arrived = lax.ppermute(rows, "tp", shift_pairs(groups, step))
        owner = (index - step + groups) % groups
        whole = lax.dynamic_update_slice_in_dim(whole, arrived, owner * rows_dev, 0)
    return whole


def sum_groups(partial, groups):
    total = partial.astype(jnp.float32)
    for step in range(1, groups):
        arrived = lax.ppermute(partial, "tp", shift_pairs(groups, step))
        total = total + arrived.astype(jnp.float32)
    return total


def scatter_groups(partial, groups, index):
    rows_dev = partial.shape[0] // groups
    total = lax.dynamic_slice_in_dim(partial, index * rows_dev, rows_dev, 0).astype(jnp.float32)
    for step in range(1, groups):
        target = (index + step) % groups
        leaving = lax.dynamic_slice_in_dim(partial, target * rows_dev, rows_dev, 0)
        arrived = lax.ppermute(leaving, "tp", shift_pairs(groups, step))
        total = total + arrived.astype(jnp.float32)
    return total


def shared_width(columns, unit, numerator, denominator):
    if lax.axis_size("rep") != 2:
        return 0
    return (columns // unit) * numerator // denominator * unit


def column_pieces(array, width):
    columns = array.shape[-1]
    if width == 0:
        return [array]
    rep_index = lax.axis_index("rep")
    pieces = [lax.dynamic_slice_in_dim(array, rep_index * (columns - width), width, array.ndim - 1)]
    if columns > 2 * width:
        pieces.append(array[..., width : columns - width])
    pieces.append(
        lax.dynamic_slice_in_dim(
            array, (1 - rep_index) * (columns - width), width, array.ndim - 1
        )
    )
    return pieces


def gather_weights(weights, width):
    columns = weights[0].shape[1]
    if width == 0:
        return [[lax.all_gather(weight, "fs", axis=0, tiled=True)] for weight in weights]
    rep_index = lax.axis_index("rep")
    start = rep_index * (columns - width)
    count = len(weights)

    def cut(whole):
        each = whole.shape[1] // count
        return [whole[:, order * each : (order + 1) * each] for order in range(count)]

    own = join([lax.dynamic_slice_in_dim(weight, start, width, 1) for weight in weights])
    first = lax.all_gather(own, "fs", axis=0, tiled=True)
    pieces = [cut(first)]
    if columns > 2 * width:
        common = join([weight[:, width : columns - width] for weight in weights])
        pieces.append(cut(lax.all_gather(common, "fs", axis=0, tiled=True)))
    pieces.append(cut(lax.ppermute(first, "rep", [(0, 1), (1, 0)])))
    return [list(each) for each in zip(*pieces)]


def product(rows_in, weight):
    return jnp.dot(rows_in, weight, preferred_element_type=jnp.float32).astype(jnp.bfloat16)


def join(pieces):
    return pieces[0] if len(pieces) == 1 else jnp.concatenate(pieces, axis=-1)


def shards_any(
    tokens,
    mix_gain,
    query_weight,
    key_weight,
    value_weight,
    gate_weight,
    out_weight,
    head_gain,
    channel_gain,
    inner_gate,
    inner_lift,
    inner_down,
    filter_taps,
    filter_bias,
):
    tp_index = lax.axis_index("tp")
    groups = lax.axis_size("tp")
    rows_dev = tokens.shape[0]
    cols_dev = query_weight.shape[1]
    hidden_dev = inner_gate.shape[1]
    heads_dev = cols_dev // HEAD_DIM
    full_length = rows_dev * groups
    head_width = shared_width(cols_dev, HEAD_DIM, 1, 2)
    hidden_width = shared_width(hidden_dev, 128, 1, 3)
    query_set, key_set = gather_weights([query_weight, key_weight], head_width)
    value_set, gate_set = gather_weights([value_weight, gate_weight], head_width)
    (out_set,) = gather_weights([out_weight], head_width)
    inner_gate_set, inner_lift_set = gather_weights([inner_gate, inner_lift], hidden_width)
    (down_set,) = gather_weights([inner_down], hidden_width)
    whole_tokens = gather_rows(tokens, groups, tp_index)
    normed_whole = lax.optimization_barrier(
        rms_scale(whole_tokens.astype(jnp.float32), mix_gain).astype(jnp.bfloat16)
    )
    queries = join([product(normed_whole, piece) for piece in query_set])
    key_rows = join([product(normed_whole, piece) for piece in key_set])
    value_rows = join([product(normed_whole, piece) for piece in value_set])
    gate_in = join([product(normed_whole, piece) for piece in gate_set])
    positions = jnp.arange(full_length, dtype=jnp.float32)
    q_rot = (
        rotate(queries.astype(jnp.float32).reshape(full_length, heads_dev, HEAD_DIM), positions)
        * HEAD_DIM ** (-0.5)
    ).astype(jnp.bfloat16)
    k_rot = rotate(
        key_rows.astype(jnp.float32).reshape(full_length, heads_dev, HEAD_DIM), positions
    ).astype(jnp.bfloat16)
    head_order = join(
        column_pieces(jnp.arange(heads_dev, dtype=jnp.int32), head_width // HEAD_DIM)
    )
    head_ids = (tp_index * heads_dev + head_order).astype(jnp.float32)
    log_gamma = jnp.log(1.0 - 2.0 ** (-5.0 - head_ids))
    retained = retain(
        q_rot, k_rot, value_rows.reshape(full_length, heads_dev, HEAD_DIM), log_gamma, BLOCK
    )
    mean_square = jnp.mean(retained * retained, axis=-1, keepdims=True)
    gain_dev = lax.dynamic_slice_in_dim(head_gain, tp_index * cols_dev, cols_dev, 0)
    gain_dev = join(column_pieces(gain_dev, head_width))
    head_normed = (retained * lax.rsqrt(mean_square + head_eps)).reshape(
        full_length, cols_dev
    ) * gain_dev
    mixed = (jax.nn.silu(gate_in.astype(jnp.float32)) * head_normed).astype(jnp.bfloat16)
    out_product = 0.0
    column = 0
    for piece in out_set:
        part = mixed[:, column : column + piece.shape[1]]
        out_product = out_product + transposed_product(part, piece)
        column += piece.shape[1]
    mixer_whole = sum_groups(out_product.astype(jnp.bfloat16), groups)
    middle_whole = whole_tokens.astype(jnp.float32) + mixer_whole
    normed_mid = lax.optimization_barrier(
        rms_scale(middle_whole, channel_gain).astype(jnp.bfloat16)
    )
    middle = lax.dynamic_slice_in_dim(middle_whole, tp_index * rows_dev, rows_dev, 0)
    taps_dev = lax.dynamic_slice_in_dim(filter_taps, tp_index * hidden_dev, hidden_dev, 1)
    bias_dev = lax.dynamic_slice_in_dim(filter_bias, tp_index * hidden_dev, hidden_dev, 0)
    taps_set = column_pieces(taps_dev, hidden_width)
    bias_set = column_pieces(bias_dev, hidden_width)
    down_product = 0.0
    for gate_piece, lift_piece, down_piece, taps_piece, bias_piece in zip(
        inner_gate_set, inner_lift_set, down_set, taps_set, bias_set
    ):
        gate_pre = product(normed_mid, gate_piece)
        lifted = product(normed_mid, lift_piece)
        padded = jnp.pad(gate_pre, ((TAPS - 1, 0), (0, 0)))
        filtered = bias_piece[None, :]
        for offset in range(TAPS):
            shifted = padded[offset : offset + full_length].astype(jnp.float32)
            filtered = filtered + shifted * taps_piece[offset][None, :]
        hidden = (jax.nn.silu(filtered) * lifted.astype(jnp.float32)).astype(jnp.bfloat16)
        down_product = down_product + transposed_product(hidden, down_piece)
    outcome = middle + scatter_groups(down_product.astype(jnp.bfloat16), groups, tp_index)
    return outcome.astype(jnp.bfloat16)


def ring_pairs(count):
    order = list(range(0, count, 2)) + list(range(count - 1, 0, -2))
    return order, [(order[at], order[(at + 1) % count]) for at in range(count)]


def after(array, *earlier):
    return lax.optimization_barrier((array,) + earlier)[0]


class Ring:
    def __init__(self, shard, count, far_way):
        _, ahead = ring_pairs(count)
        behind = [(target, source) for source, target in ahead]
        self.blocks = {0: shard}
        self.hops = []
        up = down = shard
        for step in range(1, count // 2 + 1):
            arrived = []
            for way in ways(step, count, far_way):
                if way == "up":
                    up = lax.ppermute(up, "fs", ahead)
                    self.blocks[count - step] = up
                    arrived.append(up)
                else:
                    down = lax.ppermute(down, "fs", behind)
                    self.blocks[step] = down
                    arrived.append(down)
            self.hops.append(tuple(arrived))

    def parts(self, distances):
        return [self.blocks[at] for at in distances]


def ways(step, count, far_way):
    return ("up", "down") if step < count // 2 else (far_way,)


FAR_WAY = {"ra": "up", "rb": "down", "rg": "up", "rl": "down", "rc": "up", "rd": "down"}


def swap(array, axis):
    return lax.ppermute(array, axis, [(0, 1), (1, 0)])


def retain_kernel(
    swapped_ref,
    log_gamma_ref,
    query_ref,
    key_ref,
    value_ref,
    gate_ref,
    cosine_ref,
    sine_ref,
    gain_ref,
    mixed_ref,
):
    log_gamma = log_gamma_ref[pl.program_id(0)]
    length, width = query_ref.shape
    late = swapped_ref[0] * (length // 2)
    half = width // 2
    span = BLOCK
    rows = lax.broadcasted_iota(jnp.int32, (span, span), 0)
    columns = lax.broadcasted_iota(jnp.int32, (span, span), 1)
    distance = (rows - columns).astype(jnp.float32)
    inside = jnp.where(distance >= 0, jnp.exp(jnp.maximum(distance, 0.0) * log_gamma), 0.0)
    offsets = lax.broadcasted_iota(jnp.int32, (span, width), 0).astype(jnp.float32)
    query_decay = jnp.exp((offsets + 1.0) * log_gamma)
    key_decay = jnp.exp((span - 1.0 - offsets) * log_gamma)
    span_decay = jnp.exp(jnp.full((width, width), span, jnp.float32) * log_gamma)
    gain = gain_ref[...]

    def turn(ref, at, stored, scale):
        rows_in = ref[stored, :].astype(jnp.float32)
        front, back = rows_in[:, :half], rows_in[:, half:]
        cosine = cosine_ref[pl.ds(at, span), :]
        sine = sine_ref[pl.ds(at, span), :]
        turned = jnp.concatenate(
            [front * cosine - back * sine, front * sine + back * cosine], axis=-1
        )
        return (turned * scale).astype(jnp.bfloat16)

    def both(wide):
        high = wide.astype(jnp.bfloat16)
        return high, (wide - high.astype(jnp.float32)).astype(jnp.bfloat16)

    def dot(left, right, left_axis, right_axis):
        return lax.dot_general(
            left,
            right,
            (((left_axis,), (right_axis,)), ((), ())),
            preferred_element_type=jnp.float32,
        )

    state = jnp.zeros((width, width), jnp.float32)
    for block in range(length // span):
        at = block * span
        first = at + late if at < length // 2 else at - late
        stored = pl.ds(pl.multiple_of(first, span), span)
        query = turn(query_ref, at, stored, HEAD_DIM ** (-0.5))
        key = turn(key_ref, at, stored, 1.0)
        value = value_ref[stored, :]
        weights = (dot(query, key, 1, 1) * inside).astype(jnp.bfloat16)
        retained = dot(weights, value, 1, 0)
        if block > 0:
            high, low = both(state)
            retained = retained + (dot(query, high, 1, 0) + dot(query, low, 1, 0)) * query_decay
        if block < length // span - 1:
            high, low = both(key.astype(jnp.float32) * key_decay)
            added = dot(high, value, 0, 0) + dot(low, value, 0, 0)
            state = state * span_decay + added
        mean_square = jnp.mean(retained * retained, axis=-1, keepdims=True)
        normed = retained * lax.rsqrt(mean_square + head_eps) * gain
        gate = gate_ref[stored, :].astype(jnp.float32)
        mixed_ref[stored, :] = (gate * jax.nn.sigmoid(gate) * normed).astype(jnp.bfloat16)


def mix_heads(query_key, value_gate, cosine, sine, gain, log_gamma, swapped):
    length, columns = value_gate.shape[0], query_key.shape[1] // 2
    heads = columns // HEAD_DIM
    front = pl.BlockSpec((length, HEAD_DIM), lambda head, *_: (0, head))
    back = pl.BlockSpec((length, HEAD_DIM), lambda head, *_: (0, head + heads))
    table = pl.BlockSpec((length, HEAD_DIM // 2), lambda head, *_: (0, 0))
    return pl.pallas_call(
        retain_kernel,
        out_shape=jax.ShapeDtypeStruct((length, columns), jnp.bfloat16),
        grid_spec=pltpu.PrefetchScalarGridSpec(
            num_scalar_prefetch=2,
            grid=(heads,),
            in_specs=[front, back, front, back, table, table]
            + [pl.BlockSpec((1, HEAD_DIM), lambda head, *_: (0, head))],
            out_specs=front,
        ),
        compiler_params=pltpu.CompilerParams(vmem_limit_bytes=VMEM_LIMIT),
        cost_estimate=pl.CostEstimate(
            flops=length * columns * (4 * BLOCK + 8 * HEAD_DIM) * 4,
            bytes_accessed=length * columns * 10,
            transcendentals=length * columns,
        ),
    )(swapped, log_gamma, query_key, query_key, value_gate, value_gate, cosine, sine, gain.reshape(1, -1))


VMEM_LIMIT = 16 * 2**20
HIDDEN_VMEM_LIMIT = 28 * 2**20


def stacked(refs):
    return jnp.concatenate([ref[...] for ref in refs], axis=0)


def whole_block(array):
    return pl.BlockSpec(
        array.shape, lambda at: (0,) * array.ndim, pipeline_mode=pl.Buffered(1)
    )


def strip(array, width):
    return pl.BlockSpec((array.shape[0], width), lambda at: (0, at))


def project_rows(row_parts, weight_blocks, columns, width=256):
    count = len(row_parts)
    part_rows, depth = row_parts[0].shape
    width = min(width, columns)

    def body(*refs):
        weight = stacked(refs[count:-1])
        for at in range(count):
            refs[-1][pl.ds(at * part_rows, part_rows), :] = jnp.dot(
                refs[at][...], weight, preferred_element_type=jnp.float32
            ).astype(jnp.bfloat16)

    return pl.pallas_call(
        body,
        out_shape=jax.ShapeDtypeStruct((count * part_rows, columns), jnp.bfloat16),
        grid=(columns // width,),
        in_specs=[whole_block(part) for part in row_parts]
        + [strip(block, width) for block in weight_blocks],
        out_specs=pl.BlockSpec((count * part_rows, width), lambda at: (0, at)),
        compiler_params=pltpu.CompilerParams(vmem_limit_bytes=VMEM_LIMIT),
        cost_estimate=pl.CostEstimate(
            flops=2 * count * part_rows * depth * columns,
            bytes_accessed=2 * (count * part_rows * (depth + columns) + depth * columns),
            transcendentals=0,
        ),
    )(*row_parts, *weight_blocks)


def project_back(depth_parts, weight_blocks, first_strip=0, tile=256):
    count = len(depth_parts)
    rows, strip_depth = depth_parts[0].shape
    columns = sum(block.shape[0] for block in weight_blocks)
    part_rows = rows // 2
    tiles = part_rows // tile
    first = first_strip // count

    def body(*refs):
        rows_in = jnp.concatenate([ref[...] for ref in refs[:count]], axis=1)
        product_tile = transposed_product(rows_in, stacked(refs[count:-2])).astype(jnp.bfloat16)

        @pl.when(pl.program_id(0) < tiles)
        def _():
            refs[-2][...] = product_tile

        @pl.when(pl.program_id(0) >= tiles)
        def _():
            refs[-1][...] = product_tile

    part = jax.ShapeDtypeStruct((part_rows, columns), jnp.bfloat16)
    return pl.pallas_call(
        body,
        out_shape=(part, part),
        grid=(2 * tiles,),
        in_specs=[pl.BlockSpec((tile, strip_depth), lambda at: (at, 0))] * count
        + [
            pl.BlockSpec(
                (block.shape[0], count * strip_depth),
                lambda at: (0, first),
                pipeline_mode=pl.Buffered(1),
            )
            for block in weight_blocks
        ],
        out_specs=(
            pl.BlockSpec((tile, columns), lambda at: (jnp.minimum(at, tiles - 1), 0)),
            pl.BlockSpec((tile, columns), lambda at: (jnp.maximum(at - tiles, 0), 0)),
        ),
        compiler_params=pltpu.CompilerParams(vmem_limit_bytes=VMEM_LIMIT),
        cost_estimate=pl.CostEstimate(
            flops=2 * rows * count * strip_depth * columns,
            bytes_accessed=2 * (rows * columns + count * strip_depth * (rows + columns)),
            transcendentals=0,
        ),
    )(*depth_parts, *weight_blocks)


def hidden_rows(mine, theirs, gate_blocks, lift_blocks, taps, bias, swapped, share, shares):
    part_rows, depth = mine.shape
    columns = gate_blocks[0].shape[1] // shares
    count = len(gate_blocks)
    width = next(width for width in (512, 384, 256, 128) if columns % width == 0)
    first_strip = share * (columns // width)

    chunk = 128

    def body(swapped_ref, mine_ref, theirs_ref, *refs):
        taps_ref, bias_ref, hidden_ref = refs[2 * count :]
        gate_weight, lift_weight = stacked(refs[:count]), stacked(refs[count : 2 * count])

        def rounded(rows_in, weight):
            wide = jnp.dot(rows_in, weight, preferred_element_type=jnp.float32)
            return wide.astype(jnp.bfloat16).astype(jnp.float32)

        def hidden_of(before, pre, lifted):
            padded = jnp.concatenate([before, pre], axis=0)
            filtered = bias_ref[...]
            for offset in range(TAPS):
                start = 8 - (TAPS - 1) + offset
                filtered = filtered + padded[start : start + pre.shape[0]] * taps_ref[offset : offset + 1, :]
            return (filtered * jax.nn.sigmoid(filtered) * lifted).astype(jnp.bfloat16)

        before = jnp.zeros((8, width), jnp.float32)
        for at, ref in enumerate((mine_ref, theirs_ref)):
            if at == 1:
                before = jnp.where(swapped_ref[0] == 0, before, 0.0)
            for first in range(0, part_rows, chunk):
                rows_in = ref[pl.ds(first, chunk), :]
                pre = rounded(rows_in, gate_weight)
                lifted = rounded(rows_in, lift_weight)
                hidden_ref[pl.ds(at * part_rows + first, chunk), :] = hidden_of(before, pre, lifted)
                before = pre[chunk - 8 :]
                if at == 0 and first == 0:
                    opening = pre[:16], lifted[:16]
        before = jnp.where(swapped_ref[0] == 1, before, 0.0)
        hidden_ref[pl.ds(0, 16), :] = hidden_of(before, *opening)

    def strip_at(rows, ahead=first_strip):
        return pl.BlockSpec((rows, width), lambda at, *_: (0, at + ahead))

    rows_spec = pl.BlockSpec(
        (part_rows, depth), lambda at, *_: (0, 0), pipeline_mode=pl.Buffered(1)
    )
    return pl.pallas_call(
        body,
        out_shape=jax.ShapeDtypeStruct((2 * part_rows, columns), jnp.bfloat16),
        grid_spec=pltpu.PrefetchScalarGridSpec(
            num_scalar_prefetch=1,
            grid=(columns // width,),
            in_specs=[rows_spec, rows_spec]
            + [strip_at(block.shape[0]) for block in gate_blocks + lift_blocks]
            + [strip_at(TAPS), strip_at(1)],
            out_specs=strip_at(2 * part_rows, 0),
        ),
        compiler_params=pltpu.CompilerParams(vmem_limit_bytes=HIDDEN_VMEM_LIMIT),
        cost_estimate=pl.CostEstimate(
            flops=8 * part_rows * depth * columns,
            bytes_accessed=4 * (part_rows * (depth + columns) + depth * columns),
            transcendentals=2 * part_rows * columns,
        ),
    )(swapped, mine, theirs, *gate_blocks, *lift_blocks, taps, bias)


def by_row_tiles(body, owners, arrays, wide, outputs, tile=128):
    rows = arrays[0].shape[0]

    def tiled(array):
        return pl.BlockSpec((tile, array.shape[1]), lambda at, *_: (at, 0))

    return pl.pallas_call(
        body,
        out_shape=outputs,
        grid_spec=pltpu.PrefetchScalarGridSpec(
            num_scalar_prefetch=1,
            grid=(rows // tile,),
            in_specs=[tiled(array) for array in arrays]
            + [pl.BlockSpec(array.shape, lambda at, *_: (0, 0)) for array in wide],
            out_specs=[tiled(array) for array in outputs],
        ),
        compiler_params=pltpu.CompilerParams(vmem_limit_bytes=VMEM_LIMIT),
        cost_estimate=pl.CostEstimate(
            flops=200 * rows * arrays[0].shape[1],
            bytes_accessed=4 * rows * arrays[0].shape[1] * (len(arrays) + len(outputs)) // 2,
            transcendentals=rows,
        ),
    )(owners, *arrays, *wide)


def block_of(owners_ref, distance, width):
    return pl.ds(pl.multiple_of(owners_ref[distance] * width, width), width)


def norm_input(tokens, gain, owners, count):
    rows, features = tokens.shape
    width = features // count

    def body(owners_ref, tokens_ref, gain_ref, normed_ref):
        wide = tokens_ref[...].astype(jnp.float32)
        factor = lax.rsqrt(jnp.mean(wide * wide, axis=-1, keepdims=True) + norm_eps)
        for at in range(count):
            taken = block_of(owners_ref, at, width)
            normed_ref[:, at * width : (at + 1) * width] = (
                tokens_ref[:, taken].astype(jnp.float32) * factor * gain_ref[:, taken]
            ).astype(jnp.bfloat16)

    outputs = [jax.ShapeDtypeStruct((rows, features), jnp.bfloat16)]
    return by_row_tiles(body, owners, [tokens], [gain[None, :]], outputs)[0]


def norm_middle(tokens, parts, gain, owners, count):
    rows, features = tokens.shape
    width = features // count

    def body(owners_ref, tokens_ref, mine_ref, theirs_ref, far_ref, gain_ref, middle_ref, normed_ref):
        squares = jnp.zeros((tokens_ref.shape[0], 1), jnp.float32)
        for at in range(count):
            placed = slice(at * width, (at + 1) * width)
            taken = block_of(owners_ref, at, width)
            mixer = mine_ref[:, placed].astype(jnp.float32) + theirs_ref[:, placed].astype(jnp.float32)
            mixer = mixer + far_ref[:, placed].astype(jnp.float32)
            middle = tokens_ref[:, taken].astype(jnp.float32) + mixer
            middle_ref[:, placed] = middle
            squares = squares + jnp.sum(middle * middle, axis=-1, keepdims=True)
        factor = lax.rsqrt(squares / features + norm_eps)
        for at in range(count):
            placed = slice(at * width, (at + 1) * width)
            taken = block_of(owners_ref, at, width)
            normed_ref[:, placed] = (middle_ref[:, placed] * factor * gain_ref[:, taken]).astype(
                jnp.bfloat16
            )

    outputs = [
        jax.ShapeDtypeStruct((rows, features), jnp.float32),
        jax.ShapeDtypeStruct((rows, features), jnp.bfloat16),
    ]
    return by_row_tiles(body, owners, [tokens] + parts, [gain[None, :]], outputs)


def outcome_rows(middle, group_parts, groups, owners, count):
    rows, features = middle.shape
    width = features // count
    parts = [part for group in group_parts for part in group]

    def body(owners_ref, middle_ref, *refs):
        for number, group in enumerate(groups):
            mine_ref, theirs_ref, far_ref = refs[3 * number : 3 * number + 3]
            for order, at in enumerate(group):
                placed = slice(order * width, (order + 1) * width)
                channel = mine_ref[:, placed].astype(jnp.float32) + theirs_ref[:, placed].astype(jnp.float32)
                channel = channel + far_ref[:, placed].astype(jnp.float32)
                refs[-1][:, block_of(owners_ref, at, width)] = (
                    middle_ref[:, at * width : (at + 1) * width] + channel
                ).astype(jnp.bfloat16)

    outputs = [jax.ShapeDtypeStruct((rows, features), jnp.bfloat16)]
    return by_row_tiles(body, owners, [middle] + parts, [], outputs)[0]


def shards(
    tokens,
    mix_gain,
    query_weight,
    key_weight,
    value_weight,
    gate_weight,
    out_weight,
    head_gain,
    channel_gain,
    inner_gate,
    inner_lift,
    inner_down,
    filter_taps,
    filter_bias,
):
    tp_index = lax.axis_index("tp")
    rep_index = lax.axis_index("rep")
    fs_index = lax.axis_index("fs")
    count = lax.axis_size("fs")
    odd = fs_index % 2
    place = jnp.where(odd == 0, fs_index // 2, count - 1 - fs_index // 2)
    rows_dev, _ = tokens.shape
    length = rows_dev * 2
    cols = query_weight.shape[1] // 2
    hidden_cols = inner_gate.shape[1] // 2
    heads = cols // HEAD_DIM
    every = list(range(count))
    around = (place + jnp.arange(count, dtype=jnp.int32)) % count
    owners = jnp.where(around < count // 2, 2 * around, 2 * (count - around) - 1).astype(jnp.int32)
    swapped = tp_index.reshape(1).astype(jnp.int32)

    def part(weight, columns):
        return lax.dynamic_slice_in_dim(weight, rep_index * columns, columns, weight.ndim - 1)

    def joint(pieces):
        return jnp.concatenate(pieces, axis=-1)

    ring_a = Ring(joint([part(query_weight, cols), part(key_weight, cols)]), count, FAR_WAY["ra"])
    ring_b = Ring(
        joint([part(value_weight, cols), part(gate_weight, cols), part(out_weight, cols)]),
        count,
        FAR_WAY["rb"],
    )

    ring_g = Ring(after(part(inner_gate, hidden_cols), *ring_a.hops[-1]), count, FAR_WAY["rg"])
    ring_l = Ring(after(part(inner_lift, hidden_cols), *ring_b.hops[-1]), count, FAR_WAY["rl"])
    down = part(inner_down, hidden_cols)
    down_half = down.shape[0] // 2
    ring_c = Ring(after(down[:down_half], *ring_g.hops[-1]), count, FAR_WAY["rc"])
    ring_d = Ring(after(down[down_half:], *ring_l.hops[-1]), count, FAR_WAY["rd"])

    normed = norm_input(tokens, mix_gain, owners, count)
    far = swap(normed, "rep")
    own_in = [normed, swap(normed, "tp")]
    other_in = [far, swap(far, "tp")]

    positions = jnp.arange(length, dtype=jnp.float32)
    inverse = rope_base ** (
        -jnp.arange(HEAD_DIM // 2, dtype=jnp.float32) / (HEAD_DIM // 2)
    )
    angles = positions[:, None] * inverse[None, :]
    first_head = (tp_index * 2 + rep_index) * heads
    head_ids = (first_head + jnp.arange(heads, dtype=jnp.int32)).astype(jnp.float32)
    log_gamma = jnp.log(1.0 - 2.0 ** (-5.0 - head_ids))
    gain_dev = lax.dynamic_slice_in_dim(head_gain, first_head * HEAD_DIM, cols, 0)
    first_hidden = (tp_index * 2 + rep_index) * hidden_cols

    taps = lax.dynamic_slice_in_dim(filter_taps, first_hidden, hidden_cols, 1)
    bias = lax.dynamic_slice_in_dim(filter_bias, first_hidden, hidden_cols, 0)[None, :]
    gain_dev, taps, bias = lax.optimization_barrier((gain_dev, taps, bias))
    tables = (jnp.cos(angles), jnp.sin(angles), gain_dev, log_gamma, swapped)
    early_blocks, late_blocks = ring_a.parts(every), ring_b.parts(every)

    def mixer_part(rows_in):
        query_key = project_rows(rows_in, early_blocks, 2 * cols)
        value_gate = project_rows(rows_in, late_blocks, 2 * cols)
        mixed = mix_heads(query_key, value_gate, *tables)
        return project_back([mixed], late_blocks, 2)

    other_mine, other_theirs = mixer_part(other_in)
    other_sum = other_mine.astype(jnp.float32) + swap(other_theirs, "tp").astype(jnp.float32)
    far = swap(other_sum.astype(jnp.bfloat16), "rep")
    own_mine, own_theirs = mixer_part(own_in)
    middle, normed_mid = norm_middle(
        tokens, [own_mine, swap(own_theirs, "tp"), far], channel_gain, owners, count
    )
    far = swap(normed_mid, "rep")
    own_mid = [normed_mid, swap(normed_mid, "tp")]
    other_mid = [far, swap(far, "tp")]

    hidden_blocks = ring_g.parts(every), ring_l.parts(every)

    def hidden_strips(rows_in, shares):
        return [
            hidden_rows(*rows_in, *hidden_blocks, taps, bias, swapped, share, shares)
            for share in range(shares)
        ]

    own_hidden = hidden_strips(own_mid, 1)
    other_hidden = hidden_strips(other_mid, 1)
    near = count // 2 - 2
    groups = [
        [at for at in every if min(at, count - at) <= near],
        [at for at in every if min(at, count - at) > near],
    ]
    group_parts = []
    for group in groups:
        blocks = [
            piece for at in group for ring in (ring_c, ring_d) for piece in ring.parts([at])
        ]
        other_mine, other_theirs = project_back(other_hidden, blocks)
        theirs = swap(other_theirs, "tp")
        other_sum = other_mine.astype(jnp.float32) + theirs.astype(jnp.float32)
        far = swap(other_sum.astype(jnp.bfloat16), "rep")
        own_mine, own_theirs = project_back(own_hidden, blocks)
        group_parts.append([own_mine, swap(own_theirs, "tp"), far])
    return outcome_rows(middle, group_parts, groups, owners, count)


def split_pays(mesh):
    sizes = mesh.shape
    return sizes["rep"] == 2 and sizes["tp"] == 2 and sizes["fs"] % 2 == 0 and sizes["fs"] >= 8


def solution(mesh):
    in_specs = (
        P(("rep", "fs", "tp"), None),
        P(),
        P("fs", "tp"),
        P("fs", "tp"),
        P("fs", "tp"),
        P("fs", "tp"),
        P("fs", "tp"),
        P(),
        P(),
        P("fs", "tp"),
        P("fs", "tp"),
        P("fs", "tp"),
        P(),
        P(),
    )
    out_specs = P(("rep", "fs", "tp"), None)
    if not split_pays(mesh):
        return jax.shard_map(
            shards_any, mesh=mesh, in_specs=in_specs, out_specs=out_specs, check_vma=False
        )
    return jax.shard_map(shards, mesh=mesh, in_specs=in_specs, out_specs=out_specs, check_vma=False)
```
